768 devices in a mesh: fs: 192 (over z, y, core), tp: 4 (over x).
Axes of the slice: x: 4, y: 8, z: 12, core: 2. Of those that a mesh axis runs over, the one named last changes fastest.
Arguments:
- saved_input: bfloat16 [98304, 3072], P('fs'), may hold values from -6 to 6
- output_cotangent: bfloat16 [98304, 3072], P('fs'), may hold values from -6 to 6
- recurrent_output: bfloat16 [98304, 1536], P('fs', 'tp'), may hold values from -6 to 6
- forget_logit: bfloat16 [98304, 1536], P('fs', 'tp'), may hold values from -12 to 12
- forget_cotangent: bfloat16 [98304, 1536], P('fs', 'tp'), may hold values from -6 to 6
- lower_bound: float32 [1536], P('tp'), may hold values from 0.2 to 0.9
- basis_in: bfloat16 [3072, 384], P('fs'), may hold values from -1.2629537 to 1.2629537
- basis_out: bfloat16 [3072, 384], P('fs'), may hold values from -1.2629537 to 1.2629537
- moment_in: float32 [384, 1536], P('fs', 'tp'), may hold values from -6 to 6
- second_in: float32 [384, 1536], P('fs', 'tp'), may hold values from 0.25 to 4
- moment_out: float32 [384, 1536], P('fs', 'tp'), may hold values from -6 to 6
- second_out: float32 [384, 1536], P('fs', 'tp'), may hold values from 0.25 to 4
- weight_in: float32 [3072, 1536], P('fs', 'tp'), may hold values from -0.109375 to 0.109375
- weight_out: float32 [1536, 3072], P('tp', 'fs'), may hold values from -0.15625 to 0.15625
Outputs:
- moment_in_new: float32 [384, 1536], P('fs', 'tp')
- second_in_new: float32 [384, 1536], P('fs', 'tp')
- moment_out_new: float32 [384, 1536], P('fs', 'tp')
- second_out_new: float32 [384, 1536], P('fs', 'tp')
- weight_in_new: float32 [3072, 1536], P('fs', 'tp')
- weight_out_new: float32 [1536, 3072], P('tp', 'fs')
- copy_in: bfloat16 [3072, 1536], P(None, 'tp')
- copy_out: bfloat16 [1536, 3072], P('tp')
The draws below stay inside these ranges and needn't reach their ends.
All inputs are finite; a program needn't handle non-finite values.
Results may differ from the reference program's by a relative error of at most 0.0023.
Values may be sent and summed in bfloat16 or wider, within the bound.
No kernel may reach another device: no remote copies, remote signals or barrier semaphores. Data moves between devices by JAX's collectives and lax.ppermute only.
A program may use at most 64 MiB of HBM per device.

```python
import math
import jax
import jax.numpy as jnp
from jax import lax

D = 3072
HW = 1536
R = 384
TOKENS = 98304


def scaled_basis(key):
    first, second = jax.random.split(key)
    ramp = 10.0 ** (jnp.arange(R, dtype=jnp.float32) / R)
    jitter = jax.random.uniform(first, (R,), jnp.float32, 0.7, 1.4)
    values = jnp.clip(jax.random.normal(second, (D, R), jnp.float32), -5.0, 5.0)
    return (values * ramp[None, :] * jitter[None, :] * D ** (-0.5)).astype(jnp.bfloat16)


def draw_basis_in(key, part):
    return scaled_basis(jax.random.fold_in(key, 11))


def draw_basis_out(key, part):
    return scaled_basis(jax.random.fold_in(key, 23))


def levels(rng, shape, cuts, smallest, top_value):
    level = 1.0
    for position, blocks in cuts:
        steps = jax.random.uniform(jax.random.fold_in(jax.random.fold_in(rng, 6), position), (blocks,), jnp.float32, smallest / len(cuts), top_value / len(cuts))
        level = level * jnp.repeat(jnp.exp(steps), shape[position] // blocks).reshape((-1,) + (1,) * (len(shape) - 1 - position))
    return level


def centred(key, extent, scale, most, cuts=(), held_as=jnp.bfloat16):
    values = jax.random.normal(key, extent, jnp.float32) * scale
    if len(cuts) > 0:
        values = levels(key, extent, cuts, -0.22, 0.18) * values
    return jnp.clip(values, min=-most, max=most).astype(held_as)


def setup_inputs(seed: int = 0) -> dict:
    key_of = jax.random.split(jax.random.key(seed), 15)
    saved_input = centred(key_of[0], (TOKENS, D), 1.0, 6.0, ((0, 192),))
    output_cotangent = centred(key_of[1], (TOKENS, D), 1.0, 6.0, ((0, 192),))
    recurrent_output = centred(key_of[2], (TOKENS, HW), 1.0, 6.0, ((0, 192), (1, 4)))
    forget_logit = centred(key_of[3], (TOKENS, HW), 2.0, 12.0, ((0, 192), (1, 4)))
    forget_cotangent = centred(key_of[4], (TOKENS, HW), 1.0, 6.0, ((0, 192), (1, 4)))
    lower_bound = jnp.clip(0.2 + 0.7 * jax.random.uniform(key_of[5], (HW,), jnp.float32) ** levels(key_of[5], (HW,), ((0, 4),), -0.2, 0.2), 0.2, 0.9)
    basis_in = draw_basis_in(jax.random.fold_in(key_of[14], 71), 0)
    basis_out = draw_basis_out(jax.random.fold_in(key_of[14], 71), 0)
    moment_in = centred(key_of[8], (R, HW), 1.0, 6.0, ((0, 192), (1, 4)), jnp.float32)
    second_in = jnp.clip(jnp.exp(math.log(4.0) - 2.7725887 * jax.random.uniform(key_of[9], (R, HW), jnp.float32) ** levels(key_of[9], (R, HW), ((0, 192), (1, 4)), -0.2, 0.2)), 0.25, 4.0)
    moment_out = centred(key_of[10], (R, HW), 1.0, 6.0, ((0, 192), (1, 4)), jnp.float32)
    second_out = jnp.clip(jnp.exp(math.log(4.0) - 2.7725887 * jax.random.uniform(key_of[11], (R, HW), jnp.float32) ** levels(key_of[11], (R, HW), ((0, 192), (1, 4)), -0.2, 0.2)), 0.25, 4.0)
    weight_in = centred(key_of[12], (D, HW), D ** -0.5, 0.109375, ((0, 192), (1, 4)), jnp.float32)
    weight_out = centred(key_of[13], (HW, D), HW ** -0.5, 0.15625, ((0, 4), (1, 192)), jnp.float32)
    return {"saved_input": saved_input, "output_cotangent": output_cotangent, "recurrent_output": recurrent_output, "forget_logit": forget_logit, "forget_cotangent": forget_cotangent, "lower_bound": lower_bound, "basis_in": basis_in, "basis_out": basis_out, "moment_in": moment_in, "second_in": second_in, "moment_out": moment_out, "second_out": second_out, "weight_in": weight_in, "weight_out": weight_out}


def reference(saved_input, output_cotangent, recurrent_output, forget_logit, forget_cotangent, lower_bound, basis_in, basis_out, moment_in, second_in, moment_out, second_out, weight_in, weight_out):
    sig = jax.nn.sigmoid(forget_logit.astype(jnp.float32))
    gate_cot = (forget_cotangent.astype(jnp.float32) * (1.0 - lower_bound)[None, :] * sig * (1.0 - sig)).astype(jnp.bfloat16)
    coded_in = jnp.dot(saved_input, basis_in, preferred_element_type=jnp.float32).astype(jnp.bfloat16)
    coded_out = jnp.dot(output_cotangent, basis_out, preferred_element_type=jnp.float32).astype(jnp.bfloat16)
    low_in = jnp.dot(coded_in.T, gate_cot, preferred_element_type=jnp.float32)
    low_out = jnp.dot(coded_out.T, recurrent_output, preferred_element_type=jnp.float32)
    total = jnp.sum(low_in * low_in) + jnp.sum(low_out * low_out)
    clip = jnp.minimum(1.0, jnp.sqrt(jnp.float32(2 * R * HW)) * lax.rsqrt(total + 1e-06))
    grad_in = clip * low_in
    grad_out = clip * low_out
    moment_in_new = 0.8 * moment_in + 0.2 * grad_in
    moment_out_new = 0.8 * moment_out + 0.2 * grad_out
    second_in_new = 0.9 * second_in + 0.1 * grad_in * grad_in
    second_out_new = 0.9 * second_out + 0.1 * grad_out * grad_out
    step_in = moment_in_new / (jnp.sqrt(second_in_new) + 1e-08)
    step_out = moment_out_new / (jnp.sqrt(second_out_new) + 1e-08)
    update_in = jnp.dot(basis_in.astype(jnp.float32), step_in, precision=lax.Precision.HIGHEST)
    update_out = jnp.dot(step_out.T, basis_out.astype(jnp.float32).T, precision=lax.Precision.HIGHEST)
    weight_in_new = weight_in - 0.01 * update_in
    weight_out_new = weight_out - 0.01 * update_out
    return (moment_in_new, second_in_new, moment_out_new, second_out_new, weight_in_new, weight_out_new, weight_in_new.astype(jnp.bfloat16), weight_out_new.astype(jnp.bfloat16))
```

```python
import functools

import jax
import jax.numpy as jnp
import numpy as np
from jax import lax
from jax.experimental import pallas as pl
from jax.experimental.pallas import tpu as pltpu
from jax.sharding import Mesh
from jax.sharding import PartitionSpec as P

HW = 1536
R = 384
Z, Y, C, X = "fs_0", "fs_1", "fs_2", "tp"
FS = (Z, Y, C)
F32, BF16 = jnp.float32, jnp.bfloat16


def rank_orders(n_z, n_y, n_c):
    n_fs = n_z * n_y * n_c
    at = np.arange(R)
    steps = 2 * (at % n_fs) + at // n_fs
    c, y, p, z = np.unravel_index(at, (n_c, n_y, 2, n_z))
    return steps, 2 * ((z * n_y + y) * n_c + c) + p


def dot(a, b, dims):
    return lax.dot_general(a, b, (dims, ((), ())), preferred_element_type=F32)


NN, NT = ((1,), (0,)), ((1,), (1,))


def halves(a):
    high = a.astype(BF16)
    return high, (a - high.astype(F32)).astype(BF16)


def twice(a):
    return jnp.concatenate([a, a], axis=1)


def call(kernel, args, out_shape, scratch=(), flops=10**6, **more):
    return pl.pallas_call(
        kernel,
        out_shape=out_shape,
        scratch_shapes=scratch,
        cost_estimate=pl.CostEstimate(flops=flops, bytes_accessed=10**5, transcendentals=0),
        **more,
    )(*args)


def pack_kernel(
    quarters_ref,
    after_ref,
    in_ref,
    out_ref,
    m_in_ref,
    m_out_ref,
    s_in_ref,
    s_out_ref,
    w_in_ref,
    w_out_ref,
    block_ref,
    sorted_ref,
    rows_ref,
    state,
):
    n_x, wide = quarters_ref.shape
    mine = lax.broadcasted_iota(jnp.int32, (n_x, wide), 0) == lax.axis_index(X)
    ranks = jnp.sum(jnp.where(mine, quarters_ref[...], 0.0), axis=0, keepdims=True)
    rank = lax.broadcasted_iota(jnp.int32, (R, wide), 0).astype(F32)
    lane = lax.broadcasted_iota(jnp.int32, (R, wide), 1)
    hot = jnp.where(rank == ranks, 1.0, 0.0)
    hot_in = jnp.where(lane < wide // 2, hot, 0.0).astype(BF16)
    hot_out = jnp.where(lane < wide // 2, 0.0, hot).astype(BF16)
    block_ref[...] = (dot(in_ref[...], hot_in, NN) + dot(out_ref[...], hot_out, NN)).astype(BF16)
    rank = lax.broadcasted_iota(jnp.int32, (R, R), 0).astype(F32)
    hot = jnp.where(rank == after_ref[...], 1.0, 0.0).astype(BF16)
    own = in_ref.shape[0]
    for k, ref in enumerate((in_ref, out_ref)):
        piece = dot(ref[...], hot, NN).astype(BF16)
        sorted_ref[k * own : (k + 1) * own] = piece
        rows_ref[:, k * R : (k + 1) * R] = piece
    for k, piece in enumerate(halves(w_in_ref[...])):
        rows_ref[:, (2 + k) * R : (3 + k) * R] = piece
    for k, piece in enumerate(halves(w_out_ref[...])):
        rows_ref[:, (4 + k) * R : (5 + k) * R] = piece
    for k, ref in enumerate((m_in_ref, m_out_ref, s_in_ref, s_out_ref)):
        high = ref[...].astype(BF16).astype(F32)
        state[4 * k : 4 * k + 2] = high
        state[4 * k + 2 : 4 * k + 4] = ref[...] - high
    rows_ref[:, 6 * R :] = state[...].astype(BF16)


def terms_kernel(coded_ref, logit_ref, cot_ref, rec_ref, bound_ref, term_ref):
    sig = jax.nn.sigmoid(logit_ref[...].astype(F32))
    gate_cot = (
        cot_ref[...].astype(F32) * (1.0 - bound_ref[...][None, :]) * sig * (1.0 - sig)
    ).astype(BF16)
    n_x, wide, _ = coded_ref.shape
    units, width = rec_ref.shape[1], wide // 2
    per = n_x // term_ref.shape[0]
    for k in range(n_x):
        at = k % per * width
        term_ref[k // per, at : at + width, :units] = dot(coded_ref[k, :width], gate_cot, NN)
        term_ref[k // per, at : at + width, units:] = dot(
            coded_ref[k, width:], rec_ref[...], NN
        )


def update_kernel(
    clip_ref,
    low_ref,
    state_ref,
    rows_ref,
    sorted_ref,
    w_in_ref,
    w_out_ref,
    copy_in_ref,
    copy_out_ref,
    w_in_new_ref,
    w_out_new_ref,
    state,
    low,
    step,
    step_in,
    step_out,
):
    units = w_in_ref.shape[1]

    @pl.when(pl.program_id(0) == 0)
    def _():
        count, half = state.shape[1] // 16, R // 2
        clip = clip_ref[0, 0]
        for lane in range(0, units, 128):
            state[lane // 128] = state_ref[:, lane : lane + 128].astype(F32)
        n_z, blocks = count // 16, 16
        for lane in range(0, 2 * units, 128):
            low[0, lane // 128] = low_ref[:, lane : lane + 128].astype(F32)
            for p in range(2):
                for z in range(n_z):
                    low[1, lane // 128, pl.ds(p * half + z * blocks, blocks), :] = low[
                        0, lane // 128, pl.ds(p * n_z + z, blocks, stride=2 * n_z), :
                    ]
        for side in range(2):
            for lane in range(0, units, 128):
                for p in range(2):
                    row = lambda k: state[lane // 128, pl.ds(4 * side + p + k, count, stride=16), :]
                    at, to = pl.ds(p * half, half), pl.ds(lane, 128)
                    grad = clip * low[1, (side * units + lane) // 128, at, :]
                    moment = 0.8 * (row(0) + row(2)) + 0.2 * grad
                    second = 0.9 * (row(8) + row(10)) + 0.1 * grad * grad
                    moved = 0.01 * (moment / (jnp.sqrt(second) + 1e-08))
                    step[side, at, to] = moved
        step_in[:R], step_in[R:] = halves(step[0])
        step_out[:, :R], step_out[:, R:] = halves(step[1].T)
        own = w_in_ref.shape[0]
        w_in_new_ref[...] = w_in_ref[...] - dot(twice(sorted_ref[:own]), step_in[...], NN)
        high, rest = halves(step[1])
        mine = sorted_ref[own:]
        w_out_new_ref[...] = w_out_ref[...] - (dot(mine, high, NN) + dot(mine, rest, NN))

    w = lambda k: rows_ref[:, k * R : (k + 1) * R]
    moved = dot(twice(w(0)), step_in[...], NN)
    copy_in_ref[...] = (w(2).astype(F32) + w(3).astype(F32) - moved).astype(BF16)
    moved = dot(step_out[...], twice(w(1)), NT)
    copy_out_ref[...] = ((w(4).astype(F32) + w(5).astype(F32)).T - moved).astype(BF16)


def update(clip, low, rows, sorted_both, weight_in, weight_out):
    d, units, tile = rows.shape[0], weight_in.shape[1], 512
    whole = lambda a: pl.BlockSpec(a.shape, lambda i: (0,) * a.ndim)
    return call(
        update_kernel,
        (clip, low, rows, rows, sorted_both, weight_in, weight_out),
        [
            jax.ShapeDtypeStruct((d, units), BF16),
            jax.ShapeDtypeStruct((units, d), BF16),
            jax.ShapeDtypeStruct(weight_in.shape, F32),
            jax.ShapeDtypeStruct(weight_out.shape, F32),
        ],
        scratch=[
            pltpu.VMEM((units // 128, d, 128), F32),
            pltpu.VMEM((2, 2 * units // 128, R, 128), F32),
            pltpu.VMEM((2, R, units), F32),
            pltpu.VMEM((2 * R, units), BF16),
            pltpu.VMEM((units, 2 * R), BF16),
        ],
        flops=14 * d * R * units,
        grid=(d // tile,),
        in_specs=[
            pl.BlockSpec(memory_space=pltpu.SMEM),
            whole(low),
            pl.BlockSpec((d, R), lambda i: (0, 6)),
            pl.BlockSpec((tile, 6 * R), lambda i: (i, 0)),
            whole(sorted_both),
            whole(weight_in),
            whole(weight_out),
        ],
        out_specs=[
            pl.BlockSpec((tile, units), lambda i: (i, 0)),
            pl.BlockSpec((units, tile), lambda i: (0, i)),
            whole(weight_in),
            whole(weight_out),
        ],
        compiler_params=pltpu.CompilerParams(vmem_limit_bytes=48 * 2**20),
    )


def body(
    saved_input,
    output_cotangent,
    recurrent_output,
    forget_logit,
    forget_cotangent,
    lower_bound,
    basis_in,
    basis_out,
    moment_in,
    second_in,
    moment_out,
    second_out,
    weight_in,
    weight_out,
):
    n_z, n_y, n_c, n_x = (lax.axis_size(a) for a in (Z, Y, C, X))
    n_fs = n_z * n_y * n_c
    units, own = recurrent_output.shape[1], basis_in.shape[0]
    width = R // n_x
    after, before = rank_orders(n_z, n_y, n_c)
    quarters = np.concatenate([before.reshape(n_x, width)] * 2, axis=1).astype(np.float32)
    after = after.astype(np.float32)[None, :]

    block, sorted_both, payload = call(
        pack_kernel,
        (
            jnp.asarray(quarters),
            jnp.asarray(after),
            basis_in,
            basis_out,
            moment_in,
            moment_out,
            second_in,
            second_out,
            weight_in,
            weight_out.T,
        ),
        [
            jax.ShapeDtypeStruct((own, 2 * width), BF16),
            jax.ShapeDtypeStruct((2 * own, R), BF16),
            jax.ShapeDtypeStruct((own, 7 * R), BF16),
        ],
        scratch=[pltpu.VMEM((16, units), F32)],
    )

    rows = lax.all_gather(payload, FS, axis=0, tiled=True)

    full = lax.all_gather(block, Z, axis=0, tiled=True).reshape(n_z, own, 2 * width)
    full = (full.astype(F32) * 1024.0).astype(jnp.float16)
    full = lax.all_gather(full, (Y, C), axis=0, tiled=False)
    full = jnp.moveaxis(full, 0, 1).astype(F32) * (1.0 / 1024.0)
    full = full.astype(BF16).reshape(-1, 2 * width)

    first = lax.broadcasted_iota(jnp.int32, (2 * width, 1), 0) < width
    part = jnp.where(
        first,
        dot(full, saved_input, ((0,), (1,))),
        dot(full, output_cotangent, ((0,), (1,))),
    ).astype(BF16)
    coded = lax.all_gather(part, X, axis=0, tiled=False)

    term = call(
        terms_kernel,
        (coded, forget_logit, forget_cotangent, recurrent_output, lower_bound),
        jax.ShapeDtypeStruct((n_c, R // n_c, 2 * units), F32),
        flops=4 * R * units * recurrent_output.shape[0],
    )

    term = jnp.sum(lax.all_to_all(term, C, 0, 0), axis=0)
    term = lax.all_to_all(term.reshape(n_y, -1, 2 * units), Y, 0, 0)
    term = lax.all_gather(jnp.sum(term, axis=0), Z, axis=0, tiled=False)
    term = jnp.sum(term, axis=0)
    squares = jnp.full((n_y * n_c * n_x, 128), jnp.sum(term * term))
    squares = lax.all_to_all(squares, (Y, C, X), 0, 0, tiled=True)
    low = lax.all_gather(term.astype(BF16), (Y, C), axis=0, tiled=True)
    total = jnp.sum(squares[:, 0])
    clip = jnp.minimum(1.0, jnp.sqrt(jnp.float32(2 * R * HW)) * lax.rsqrt(total + 1e-06))

    mine = [lax.dynamic_slice_in_dim(term, p * n_z + lax.axis_index(Z), 1, 0) for p in range(2)]
    mine = clip * jnp.concatenate(mine, axis=0)

    def moved(moment, second, grad):
        return 0.8 * moment + 0.2 * grad, 0.9 * second + 0.1 * grad * grad

    moment_in_new, second_in_new = moved(moment_in, second_in, mine[:, :units])
    moment_out_new, second_out_new = moved(moment_out, second_out, mine[:, units:])
    copy_in, copy_out, weight_in_new, weight_out_new = update(
        clip.reshape(1, 1), low, rows, sorted_both, weight_in, weight_out.T
    )
    weight_out_new = weight_out_new.T
    return (
        moment_in_new,
        second_in_new,
        moment_out_new,
        second_out_new,
        weight_in_new,
        weight_out_new,
        copy_in,
        copy_out,
    )


def solution(mesh):
    finer = Mesh(mesh.devices.reshape(12, 8, 2, mesh.shape["tp"]), (Z, Y, C, X))
    return jax.shard_map(
        body,
        mesh=finer,
        in_specs=(
            P(FS, None),
            P(FS, None),
            P(FS, X),
            P(FS, X),
            P(FS, X),
            P(X),
            P(FS, None),
            P(FS, None),
            P(FS, X),
            P(FS, X),
            P(FS, X),
            P(FS, X),
            P(FS, X),
            P(X, FS),
        ),
        out_specs=(
            P(FS, X),
            P(FS, X),
            P(FS, X),
            P(FS, X),
            P(FS, X),
            P(X, FS),
            P(None, X),
            P(X, None),
        ),
        check_vma=False,
    )
```

```python
import jax
import jax.numpy as jnp
import numpy as np
from jax import lax
from jax.experimental import pallas as pl
from jax.experimental.pallas import tpu as pltpu
from jax.sharding import Mesh
from jax.sharding import PartitionSpec as P

HW = 1536
R = 384
LANES = 128
SCALE = 1024.0
Z, Y, C, X = "fs_0", "fs_1", "fs_2", "tp"
FS = (Z, Y, C)
F32, BF16, F16 = jnp.float32, jnp.bfloat16, jnp.float16
NN, NT = ((1,), (0,)), ((1,), (1,))


def rank_order(n_z, n_y, n_c):
    c, y, p, z = np.unravel_index(np.arange(R), (n_c, n_y, 2, n_z))
    return 2 * ((z * n_y + y) * n_c + c) + p


def dot(a, b, dims):
    return lax.dot_general(a, b, (dims, ((), ())), preferred_element_type=F32)


def halves(a):
    high = a.astype(BF16)
    return high, (a - high.astype(F32)).astype(BF16)


def twice(a):
    return jnp.concatenate([a, a], axis=1)


def lanes(a, width):
    return jnp.concatenate([a] * (width // LANES), axis=1)


def call(kernel, args, out_shape, scratch=(), flops=10**6, **more):
    return pl.pallas_call(
        kernel,
        out_shape=out_shape,
        scratch_shapes=scratch,
        cost_estimate=pl.CostEstimate(flops=flops, bytes_accessed=10**5, transcendentals=0),
        **more,
    )(*args)


def pack_kernel(
    order_ref,
    in_ref,
    out_ref,
    m_in_ref,
    m_out_ref,
    s_in_ref,
    s_out_ref,
    w_in_ref,
    w_out_ref,
    sorted_ref,
    rows_ref,
):
    rank = lax.broadcasted_iota(jnp.int32, (R, R), 0).astype(F32)
    hot = jnp.where(rank == order_ref[...], 1.0, 0.0).astype(BF16)
    own, units = w_in_ref.shape
    for k, ref in enumerate((in_ref, out_ref)):
        piece = dot(ref[...], hot, NN)
        sorted_ref[k * own : (k + 1) * own] = piece.astype(BF16)
        rows_ref[:, k * R : (k + 1) * R] = SCALE * piece
    at = 2 * R
    for ref in (w_in_ref, w_out_ref):
        rows_ref[:, at : at + units] = SCALE * ref[...]
        at += units
    rows_ref[:, at:] = jnp.zeros((own, 2 * LANES), F32)
    for k, ref in enumerate((m_in_ref, m_out_ref, s_in_ref, s_out_ref)):
        for p in range(2):
            row = SCALE * ref[p : p + 1]
            rows_ref[4 * k + 2 * p : 4 * k + 2 * p + 1, at:] = row[:, : 2 * LANES]
            rows_ref[4 * k + 2 * p + 1 : 4 * k + 2 * p + 2, at : at + LANES] = row[:, 2 * LANES :]


def terms_kernel(in_ref, out_ref, logit_ref, cot_ref, rec_ref, bound_ref, term_ref):
    sig = jax.nn.sigmoid(logit_ref[...].astype(F32))
    gate_cot = (
        cot_ref[...].astype(F32) * (1.0 - bound_ref[...][None, :]) * sig * (1.0 - sig)
    ).astype(BF16)
    parts, rows, units = term_ref.shape[0], term_ref.shape[1], rec_ref.shape[1]
    for k in range(parts):
        term_ref[k, :, :units] = dot(in_ref[k * rows : (k + 1) * rows], gate_cot, NN)
        term_ref[k, :, units:] = dot(out_ref[k * rows : (k + 1) * rows], rec_ref[...], NN)


def summed(ref, width):
    total = 0.0
    for k in range(ref.shape[0]):
        piece = ref[k, :, :width]
        if ref.shape[2] > width:
            root = ref[k, :, width:]
            piece = piece * lanes(root * root * (1.0 / 4096.0), width)
        total = total + piece
    return total


def repack_kernel(terms_ref, packed_ref):
    width = packed_ref.shape[1] - LANES
    total = summed(terms_ref, width)
    top = jnp.maximum(jnp.max(jnp.abs(total)), 1e-08)
    root = jnp.sqrt(jnp.full((1, LANES), top, F32)).astype(BF16).astype(F32)
    packed_ref[:, :width] = total * lanes(4096.0 / (root * root), width)
    packed_ref[:, width:] = jnp.broadcast_to(root, (packed_ref.shape[0], LANES))


def totals_kernel(terms_ref, total_ref, rounded_ref, squares_ref):
    total = summed(terms_ref, total_ref.shape[1])
    total_ref[...] = total
    rounded_ref[...] = total.astype(BF16)
    squares_ref[...] = jnp.full(squares_ref.shape, jnp.sum(total * total), F32)


def update_kernel(
    squares_ref,
    low_ref,
    term_ref,
    state,
    basis_ref,
    wide_ref,
    sorted_ref,
    w_in_ref,
    w_out_ref,
    m_in_ref,
    m_out_ref,
    s_in_ref,
    s_out_ref,
    copy_in_ref,
    copy_out_ref,
    w_in_new_ref,
    w_out_new_ref,
    m_in_new_ref,
    m_out_new_ref,
    s_in_new_ref,
    s_out_new_ref,
    step,
    step_in,
    step_out,
):
    units = w_in_ref.shape[1]

    @pl.when(pl.program_id(0) == 0)
    def _():
        total = jnp.sum(squares_ref[...], axis=0)
        clip = jnp.minimum(1.0, jnp.sqrt(jnp.float32(2 * R * HW)) * lax.rsqrt(total + 1e-06))
        n_z, n_y, n_c = (lax.axis_size(a) for a in (Z, Y, C))
        blocks, rows = n_y * n_c, 2 * n_z
        for side in range(2):
            for lane in range(0, units, LANES):
                split, at_lane = divmod(lane, 2 * LANES)

                def row(k, y, c):
                    first = (y * n_c + c) * 16 + 4 * k + split
                    ranks = [
                        state[at_lane // LANES, pl.ds(first + 2 * p, n_z, stride=16 * blocks), :]
                        for p in range(2)
                    ]
                    return jnp.concatenate(ranks, axis=0) * (1.0 / SCALE)

                for y in range(n_y):
                    for c in range(n_c):
                        low = low_ref[
                            (y * n_c + c) * rows : (y * n_c + c + 1) * rows,
                            side * units + lane : side * units + lane + LANES,
                        ]
                        grad = clip * low.astype(F32)
                        moment = 0.8 * row(side, y, c) + 0.2 * grad
                        second = 0.9 * row(2 + side, y, c) + 0.1 * grad * grad
                        at = (c * n_y + y) * rows
                        step[side, at : at + rows, lane : lane + LANES] = 0.01 * (
                            moment / (jnp.sqrt(second) + 1e-08)
                        )
        step_in[:R], step_in[R:] = halves(step[0])
        step_out[:, :R], step_out[:, R:] = halves(step[1].T)
        own = w_in_ref.shape[0]
        w_in_new_ref[...] = w_in_ref[...] - dot(twice(sorted_ref[:own]), step_in[...], NN)
        high, rest = halves(step[1])
        mine = sorted_ref[own:]
        w_out_new_ref[...] = w_out_ref[...] - (dot(mine, high, NN) + dot(mine, rest, NN))
        for p in range(2):
            grad = term_ref[pl.ds(p * n_z + lax.axis_index(Z), 1), :] * lanes(clip, 2 * units)
            for g, m, s, m_new, s_new in (
                (grad[:, :units], m_in_ref, s_in_ref, m_in_new_ref, s_in_new_ref),
                (grad[:, units:], m_out_ref, s_out_ref, m_out_new_ref, s_out_new_ref),
            ):
                m_new[p : p + 1] = 0.8 * m[p : p + 1] + 0.2 * g
                s_new[p : p + 1] = 0.9 * s[p : p + 1] + 0.1 * g * g

    moved = dot(twice(basis_ref[:, :R]), step_in[...], NN)
    copy_in_ref[...] = (wide_ref[:, :units] * (1.0 / SCALE) - moved).astype(BF16)
    moved = dot(step_out[...], twice(basis_ref[:, R:]), NT)
    copy_out_ref[...] = (wide_ref[:, units:].T * (1.0 / SCALE) - moved).astype(BF16)


def update(squares, low, term, state, basis, wide, sorted_both, weight_in, weight_out, moments):
    d, units, tile = basis.shape[0], weight_in.shape[1], 512
    whole = lambda a: pl.BlockSpec(a.shape, lambda i: (0,) * a.ndim)
    like = lambda a: jax.ShapeDtypeStruct(a.shape, F32)
    small = (weight_in, weight_out, *moments)
    return call(
        update_kernel,
        (squares, low, term, state, basis, wide, sorted_both, *small),
        [
            jax.ShapeDtypeStruct((d, units), BF16),
            jax.ShapeDtypeStruct((units, d), BF16),
            *[like(a) for a in small],
        ],
        scratch=[
            pltpu.VMEM((2, R, units), F32),
            pltpu.VMEM((2 * R, units), BF16),
            pltpu.VMEM((units, 2 * R), BF16),
        ],
        flops=8 * d * R * units,
        grid=(d // tile,),
        in_specs=[
            whole(squares),
            whole(low),
            whole(term),
            whole(state),
            pl.BlockSpec((tile, 2 * R), lambda i: (i, 0)),
            pl.BlockSpec((tile, 2 * units), lambda i: (i, 0)),
            whole(sorted_both),
            *[whole(a) for a in small],
        ],
        out_specs=[
            pl.BlockSpec((tile, units), lambda i: (i, 0)),
            pl.BlockSpec((units, tile), lambda i: (0, i)),
            *[whole(a) for a in small],
        ],
        compiler_params=pltpu.CompilerParams(vmem_limit_bytes=48 * 2**20),
    )


def body(
    saved_input,
    output_cotangent,
    recurrent_output,
    forget_logit,
    forget_cotangent,
    lower_bound,
    basis_in,
    basis_out,
    moment_in,
    second_in,
    moment_out,
    second_out,
    weight_in,
    weight_out,
):
    n_z, n_y, n_c, n_x = (lax.axis_size(a) for a in (Z, Y, C, X))
    units, own = recurrent_output.shape[1], basis_in.shape[0]
    moments = (moment_in, moment_out, second_in, second_out)
    order = rank_order(n_z, n_y, n_c).astype(np.float32)[None, :]

    sorted_both, payload = call(
        pack_kernel,
        (jnp.asarray(order), basis_in, basis_out, *moments, weight_in, weight_out.T),
        [
            jax.ShapeDtypeStruct((2 * own, R), BF16),
            jax.ShapeDtypeStruct((own, 2 * R + 2 * units + 2 * LANES), F32),
        ],
    )
    rows = lax.all_gather(payload.astype(F16), FS, axis=0, tiled=True)
    basis = (rows[:, : 2 * R].astype(F32) * (1.0 / SCALE)).astype(BF16)
    wide = rows[:, 2 * R : 2 * R + 2 * units].astype(F32)
    at = 2 * R + 2 * units
    state = jnp.stack([rows[:, at : at + LANES], rows[:, at + LANES :]]).astype(F32)

    coded_in = dot(basis[:, :R], saved_input, ((0,), (1,))).astype(BF16)
    coded_out = dot(basis[:, R:], output_cotangent, ((0,), (1,))).astype(BF16)
    term = call(
        terms_kernel,
        (coded_in, coded_out, forget_logit, forget_cotangent, recurrent_output, lower_bound),
        jax.ShapeDtypeStruct((n_c, R // n_c, 2 * units), F32),
        flops=4 * R * units * recurrent_output.shape[0],
    )

    block = R // n_c // n_y

    def repacked(terms):
        shape = jax.ShapeDtypeStruct((terms.shape[1], 2 * units + LANES), F32)
        return call(repack_kernel, (terms,), shape).astype(F16)

    term = repacked(lax.all_to_all(term, C, 0, 0)).reshape(n_y, block, -1)
    term = repacked(lax.all_to_all(term, Y, 0, 0).astype(F32))
    term, rounded, squares = call(
        totals_kernel,
        (lax.all_gather(term, Z, axis=0, tiled=False).astype(F32),),
        [
            jax.ShapeDtypeStruct((block, 2 * units), F32),
            jax.ShapeDtypeStruct((block, 2 * units), BF16),
            jax.ShapeDtypeStruct((n_y * n_c * n_x, 1, LANES), F32),
        ],
    )
    squares = lax.all_to_all(squares, (Y, C, X), 0, 0, tiled=True)
    low = lax.all_gather(rounded, (Y, C), axis=0, tiled=True)
    new = update(
        squares, low, term, state, basis, wide, sorted_both, weight_in, weight_out.T, moments
    )
    copy_in, copy_out, weight_in, weight_out, moment_in, moment_out, second_in, second_out = new
    return (
        moment_in,
        second_in,
        moment_out,
        second_out,
        weight_in,
        weight_out.T,
        copy_in,
        copy_out,
    )


def solution(mesh):
    finer = Mesh(mesh.devices.reshape(12, 8, 2, mesh.shape["tp"]), (Z, Y, C, X))
    return jax.shard_map(
        body,
        mesh=finer,
        in_specs=(
            P(FS, None),
            P(FS, None),
            P(FS, X),
            P(FS, X),
            P(FS, X),
            P(X),
            P(FS, None),
            P(FS, None),
            P(FS, X),
            P(FS, X),
            P(FS, X),
            P(FS, X),
            P(FS, X),
            P(X, FS),
        ),
        out_specs=(
            P(FS, X),
            P(FS, X),
            P(FS, X),
            P(FS, X),
            P(FS, X),
            P(X, FS),
            P(None, X),
            P(X, None),
        ),
        check_vma=False,
    )
```

```python
import functools

import jax
import jax.numpy as jnp
import numpy as np
from jax import lax
from jax.experimental import pallas as pl
from jax.experimental.pallas import tpu as pltpu
from jax.sharding import Mesh
from jax.sharding import PartitionSpec as P

HW = 1536
R = 384
Z, Y, C, X = "fs_0", "fs_1", "fs_2", "tp"
FS = (Z, Y, C)
F32, BF16 = jnp.float32, jnp.bfloat16


def rank_orders(n_z, n_y, n_c):
    n_fs = n_z * n_y * n_c
    at = np.arange(R)
    steps = 2 * (at % n_fs) + at // n_fs
    c, y, p, z = np.unravel_index(at, (n_c, n_y, 2, n_z))
    return steps, 2 * ((z * n_y + y) * n_c + c) + p


def dot(a, b, dims):
    return lax.dot_general(a, b, (dims, ((), ())), preferred_element_type=F32)


NN, NT = ((1,), (0,)), ((1,), (1,))


def halves(a):
    high = a.astype(BF16)
    return high, (a - high.astype(F32)).astype(BF16)


def twice(a):
    return jnp.concatenate([a, a], axis=1)


def call(kernel, args, out_shape, scratch=(), flops=10**6, **more):
    return pl.pallas_call(
        kernel,
        out_shape=out_shape,
        scratch_shapes=scratch,
        cost_estimate=pl.CostEstimate(flops=flops, bytes_accessed=10**5, transcendentals=0),
        **more,
    )(*args)


def pack_kernel(
    quarters_ref,
    after_ref,
    in_ref,
    out_ref,
    m_in_ref,
    m_out_ref,
    s_in_ref,
    s_out_ref,
    w_in_ref,
    w_out_ref,
    block_ref,
    sorted_ref,
    rows_ref,
    state,
):
    n_x, wide = quarters_ref.shape
    mine = lax.broadcasted_iota(jnp.int32, (n_x, wide), 0) == lax.axis_index(X)
    ranks = jnp.sum(jnp.where(mine, quarters_ref[...], 0.0), axis=0, keepdims=True)
    rank = lax.broadcasted_iota(jnp.int32, (R, wide), 0).astype(F32)
    lane = lax.broadcasted_iota(jnp.int32, (R, wide), 1)
    hot = jnp.where(rank == ranks, 1.0, 0.0)
    hot_in = jnp.where(lane < wide // 2, hot, 0.0).astype(BF16)
    hot_out = jnp.where(lane < wide // 2, 0.0, hot).astype(BF16)
    block_ref[...] = (dot(in_ref[...], hot_in, NN) + dot(out_ref[...], hot_out, NN)).astype(BF16)
    rank = lax.broadcasted_iota(jnp.int32, (R, R), 0).astype(F32)
    hot = jnp.where(rank == after_ref[...], 1.0, 0.0).astype(BF16)
    own = in_ref.shape[0]
    for k, ref in enumerate((in_ref, out_ref)):
        piece = dot(ref[...], hot, NN).astype(BF16)
        sorted_ref[k * own : (k + 1) * own] = piece
        rows_ref[:, k * R : (k + 1) * R] = piece
    for k, piece in enumerate(halves(w_in_ref[...])):
        rows_ref[:, (2 + k) * R : (3 + k) * R] = piece
    for k, piece in enumerate(halves(w_out_ref[...])):
        rows_ref[:, (4 + k) * R : (5 + k) * R] = piece
    for k, ref in enumerate((m_in_ref, m_out_ref, s_in_ref, s_out_ref)):
        high = ref[...].astype(BF16).astype(F32)
        state[4 * k : 4 * k + 2] = high
        state[4 * k + 2 : 4 * k + 4] = ref[...] - high
    rows_ref[:, 6 * R :] = state[...].astype(BF16)


def terms_kernel(coded_ref, logit_ref, cot_ref, rec_ref, bound_ref, term_ref):
    sig = jax.nn.sigmoid(logit_ref[...].astype(F32))
    gate_cot = (
        cot_ref[...].astype(F32) * (1.0 - bound_ref[...][None, :]) * sig * (1.0 - sig)
    ).astype(BF16)
    n_x, wide, _ = coded_ref.shape
    units, width = rec_ref.shape[1], wide // 2
    per = n_x // term_ref.shape[0]
    for k in range(n_x):
        at = k % per * width
        term_ref[k // per, at : at + width, :units] = dot(coded_ref[k, :width], gate_cot, NN)
        term_ref[k // per, at : at + width, units:] = dot(
            coded_ref[k, width:], rec_ref[...], NN
        )


def totals_kernel(terms_ref, total_ref, rounded_ref, squares_ref):
    total = terms_ref[0].astype(F32)
    for k in range(1, terms_ref.shape[0]):
        total = total + terms_ref[k].astype(F32)
    total_ref[...] = total
    rounded_ref[...] = total.astype(BF16)
    squares_ref[...] = jnp.full(squares_ref.shape, jnp.sum(total * total), F32)


def update_kernel(
    squares_ref,
    low_ref,
    term_ref,
    state_ref,
    rows_ref,
    sorted_ref,
    w_in_ref,
    w_out_ref,
    m_in_ref,
    m_out_ref,
    s_in_ref,
    s_out_ref,
    copy_in_ref,
    copy_out_ref,
    w_in_new_ref,
    w_out_new_ref,
    m_in_new_ref,
    m_out_new_ref,
    s_in_new_ref,
    s_out_new_ref,
    state,
    low,
    step,
    step_in,
    step_out,
):
    units = w_in_ref.shape[1]

    @pl.when(pl.program_id(0) == 0)
    def _():
        count, half = state.shape[1] // 16, R // 2
        total = jnp.sum(squares_ref[...], axis=0)
        clip = jnp.minimum(1.0, jnp.sqrt(jnp.float32(2 * R * HW)) * lax.rsqrt(total + 1e-06))
        for lane in range(0, units, 128):
            state[lane // 128] = state_ref[:, lane : lane + 128].astype(F32)
        n_z, blocks = count // 16, 16
        for lane in range(0, 2 * units, 128):
            low[0, lane // 128] = low_ref[:, lane : lane + 128].astype(F32)
            for p in range(2):
                for z in range(n_z):
                    low[1, lane // 128, pl.ds(p * half + z * blocks, blocks), :] = low[
                        0, lane // 128, pl.ds(p * n_z + z, blocks, stride=2 * n_z), :
                    ]
        for side in range(2):
            for lane in range(0, units, 128):
                for p in range(2):
                    row = lambda k: state[lane // 128, pl.ds(4 * side + p + k, count, stride=16), :]
                    at, to = pl.ds(p * half, half), pl.ds(lane, 128)
                    grad = clip * low[1, (side * units + lane) // 128, at, :]
                    moment = 0.8 * (row(0) + row(2)) + 0.2 * grad
                    second = 0.9 * (row(8) + row(10)) + 0.1 * grad * grad
                    moved = 0.01 * (moment / (jnp.sqrt(second) + 1e-08))
                    step[side, at, to] = moved
        step_in[:R], step_in[R:] = halves(step[0])
        step_out[:, :R], step_out[:, R:] = halves(step[1].T)
        own = w_in_ref.shape[0]
        w_in_new_ref[...] = w_in_ref[...] - dot(twice(sorted_ref[:own]), step_in[...], NN)
        high, rest = halves(step[1])
        mine = sorted_ref[own:]
        w_out_new_ref[...] = w_out_ref[...] - (dot(mine, high, NN) + dot(mine, rest, NN))
        for p in range(2):
            grad = term_ref[pl.ds(p * n_z + lax.axis_index(Z), 1), :]
            grad = grad * jnp.concatenate([clip] * (2 * units // 128), axis=1)
            for g, m, s, m_new, s_new in (
                (grad[:, :units], m_in_ref, s_in_ref, m_in_new_ref, s_in_new_ref),
                (grad[:, units:], m_out_ref, s_out_ref, m_out_new_ref, s_out_new_ref),
            ):
                m_new[p : p + 1] = 0.8 * m[p : p + 1] + 0.2 * g
                s_new[p : p + 1] = 0.9 * s[p : p + 1] + 0.1 * g * g

    w = lambda k: rows_ref[:, k * R : (k + 1) * R]
    moved = dot(twice(w(0)), step_in[...], NN)
    copy_in_ref[...] = (w(2).astype(F32) + w(3).astype(F32) - moved).astype(BF16)
    moved = dot(step_out[...], twice(w(1)), NT)
    copy_out_ref[...] = ((w(4).astype(F32) + w(5).astype(F32)).T - moved).astype(BF16)


def update(squares, low, term, rows, sorted_both, weight_in, weight_out, moments):
    d, units, tile = rows.shape[0], weight_in.shape[1], 512
    whole = lambda a: pl.BlockSpec(a.shape, lambda i: (0,) * a.ndim)
    small = (weight_in, weight_out, *moments)
    return call(
        update_kernel,
        (squares, low, term, rows, rows, sorted_both, *small),
        [
            jax.ShapeDtypeStruct((d, units), BF16),
            jax.ShapeDtypeStruct((units, d), BF16),
            *[jax.ShapeDtypeStruct(a.shape, F32) for a in small],
        ],
        scratch=[
            pltpu.VMEM((units // 128, d, 128), F32),
            pltpu.VMEM((2, 2 * units // 128, R, 128), F32),
            pltpu.VMEM((2, R, units), F32),
            pltpu.VMEM((2 * R, units), BF16),
            pltpu.VMEM((units, 2 * R), BF16),
        ],
        flops=14 * d * R * units,
        grid=(d // tile,),
        in_specs=[
            whole(squares),
            whole(low),
            whole(term),
            pl.BlockSpec((d, R), lambda i: (0, 6)),
            pl.BlockSpec((tile, 6 * R), lambda i: (i, 0)),
            whole(sorted_both),
            *[whole(a) for a in small],
        ],
        out_specs=[
            pl.BlockSpec((tile, units), lambda i: (i, 0)),
            pl.BlockSpec((units, tile), lambda i: (0, i)),
            *[whole(a) for a in small],
        ],
        compiler_params=pltpu.CompilerParams(vmem_limit_bytes=60 * 2**20),
    )


def body(
    saved_input,
    output_cotangent,
    recurrent_output,
    forget_logit,
    forget_cotangent,
    lower_bound,
    basis_in,
    basis_out,
    moment_in,
    second_in,
    moment_out,
    second_out,
    weight_in,
    weight_out,
):
    n_z, n_y, n_c, n_x = (lax.axis_size(a) for a in (Z, Y, C, X))
    n_fs = n_z * n_y * n_c
    units, own = recurrent_output.shape[1], basis_in.shape[0]
    width = R // n_x
    after, before = rank_orders(n_z, n_y, n_c)
    quarters = np.concatenate([before.reshape(n_x, width)] * 2, axis=1).astype(np.float32)
    after = after.astype(np.float32)[None, :]

    block, sorted_both, payload = call(
        pack_kernel,
        (
            jnp.asarray(quarters),
            jnp.asarray(after),
            basis_in,
            basis_out,
            moment_in,
            moment_out,
            second_in,
            second_out,
            weight_in,
            weight_out.T,
        ),
        [
            jax.ShapeDtypeStruct((own, 2 * width), BF16),
            jax.ShapeDtypeStruct((2 * own, R), BF16),
            jax.ShapeDtypeStruct((own, 7 * R), BF16),
        ],
        scratch=[pltpu.VMEM((16, units), F32)],
    )

    rows = lax.all_gather(payload, FS, axis=0, tiled=True)

    full = lax.all_gather(block, Z, axis=0, tiled=True).reshape(n_z, own, 2 * width)
    full = (full.astype(F32) * 1024.0).astype(jnp.float16)
    full = lax.all_gather(full, (Y, C), axis=0, tiled=False)
    full = jnp.moveaxis(full, 0, 1).astype(F32) * (1.0 / 1024.0)
    full = full.astype(BF16).reshape(-1, 2 * width)

    first = lax.broadcasted_iota(jnp.int32, (2 * width, 1), 0) < width
    part = jnp.where(
        first,
        dot(full, saved_input, ((0,), (1,))),
        dot(full, output_cotangent, ((0,), (1,))),
    ).astype(BF16)
    coded = lax.all_gather(part, X, axis=0, tiled=False)

    term = call(
        terms_kernel,
        (coded, forget_logit, forget_cotangent, recurrent_output, lower_bound),
        jax.ShapeDtypeStruct((n_c, R // n_c, 2 * units), F32),
        flops=4 * R * units * recurrent_output.shape[0],
    )

    term = lax.all_to_all(term, C, 0, 0)
    term = (term[0] + term[1]).astype(BF16).reshape(n_y, R // n_c // n_y, -1)
    term = jnp.sum(lax.all_to_all(term, Y, 0, 0).astype(F32), axis=0).astype(BF16)
    term, rounded, squares = call(
        totals_kernel,
        (lax.all_gather(term, Z, axis=0, tiled=False),),
        [
            jax.ShapeDtypeStruct(term.shape, F32),
            jax.ShapeDtypeStruct(term.shape, BF16),
            jax.ShapeDtypeStruct((n_y * n_c * n_x, 1, 128), F32),
        ],
    )
    squares = lax.all_to_all(squares, (Y, C, X), 0, 0, tiled=True)
    low = lax.all_gather(rounded, (Y, C), axis=0, tiled=True)
    moments = (moment_in, moment_out, second_in, second_out)
    new = update(squares, low, term, rows, sorted_both, weight_in, weight_out.T, moments)
    copy_in, copy_out, weight_in, weight_out, moment_in, moment_out, second_in, second_out = new
    return (
        moment_in,
        second_in,
        moment_out,
        second_out,
        weight_in,
        weight_out.T,
        copy_in,
        copy_out,
    )


def solution(mesh):
    finer = Mesh(mesh.devices.reshape(12, 8, 2, mesh.shape["tp"]), (Z, Y, C, X))
    return jax.shard_map(
        body,
        mesh=finer,
        in_specs=(
            P(FS, None),
            P(FS, None),
            P(FS, X),
            P(FS, X),
            P(FS, X),
            P(X),
            P(FS, None),
            P(FS, None),
            P(FS, X),
            P(FS, X),
            P(FS, X),
            P(FS, X),
            P(FS, X),
            P(X, FS),
        ),
        out_specs=(
            P(FS, X),
            P(FS, X),
            P(FS, X),
            P(FS, X),
            P(FS, X),
            P(X, FS),
            P(None, X),
            P(X, None),
        ),
        check_vma=False,
    )
```

```python
import functools

import jax
import jax.numpy as jnp
import numpy as np
from jax import lax
from jax.experimental import pallas as pl
from jax.experimental.pallas import tpu as pltpu
from jax.sharding import Mesh
from jax.sharding import PartitionSpec as P

HW = 1536
R = 384
Z, Y, C, X = "fs_0", "fs_1", "fs_2", "tp"
FS = (Z, Y, C)
F32, BF16 = jnp.float32, jnp.bfloat16


def rank_orders(n_z, n_y, n_c):
    n_fs = n_z * n_y * n_c
    at = np.arange(R)
    steps = 2 * (at % n_fs) + at // n_fs
    c, y, p, z = np.unravel_index(at, (n_c, n_y, 2, n_z))
    return steps, 2 * ((z * n_y + y) * n_c + c) + p


def dot(a, b, dims):
    return lax.dot_general(a, b, (dims, ((), ())), preferred_element_type=F32)


NN, NT = ((1,), (0,)), ((1,), (1,))


def halves(a):
    high = a.astype(BF16)
    return high, (a - high.astype(F32)).astype(BF16)


def twice(a):
    return jnp.concatenate([a, a], axis=1)


def call(kernel, args, out_shape, scratch=(), flops=10**6, **more):
    return pl.pallas_call(
        kernel,
        out_shape=out_shape,
        scratch_shapes=scratch,
        cost_estimate=pl.CostEstimate(flops=flops, bytes_accessed=10**5, transcendentals=0),
        **more,
    )(*args)


def pack_kernel(
    quarters_ref,
    after_ref,
    in_ref,
    out_ref,
    m_in_ref,
    m_out_ref,
    s_in_ref,
    s_out_ref,
    w_in_ref,
    w_out_ref,
    block_ref,
    sorted_ref,
    rows_ref,
    state,
):
    n_x, wide = quarters_ref.shape
    mine = lax.broadcasted_iota(jnp.int32, (n_x, wide), 0) == lax.axis_index(X)
    ranks = jnp.sum(jnp.where(mine, quarters_ref[...], 0.0), axis=0, keepdims=True)
    rank = lax.broadcasted_iota(jnp.int32, (R, wide), 0).astype(F32)
    lane = lax.broadcasted_iota(jnp.int32, (R, wide), 1)
    hot = jnp.where(rank == ranks, 1.0, 0.0)
    hot_in = jnp.where(lane < wide // 2, hot, 0.0).astype(BF16)
    hot_out = jnp.where(lane < wide // 2, 0.0, hot).astype(BF16)
    block = (dot(in_ref[...], hot_in, NN) + dot(out_ref[...], hot_out, NN)).astype(BF16)
    for k in range(block_ref.shape[0]):
        block_ref[k] = block
    rank = lax.broadcasted_iota(jnp.int32, (R, R), 0).astype(F32)
    hot = jnp.where(rank == after_ref[...], 1.0, 0.0).astype(BF16)
    own = in_ref.shape[0]
    for k, ref in enumerate((in_ref, out_ref)):
        piece = dot(ref[...], hot, NN).astype(BF16)
        sorted_ref[k * own : (k + 1) * own] = piece
        rows_ref[:, k * R : (k + 1) * R] = piece
    for k, piece in enumerate(halves(w_in_ref[...])):
        rows_ref[:, (2 + k) * R : (3 + k) * R] = piece
    for k, piece in enumerate(halves(w_out_ref[...])):
        rows_ref[:, (4 + k) * R : (5 + k) * R] = piece
    for k, ref in enumerate((m_in_ref, m_out_ref, s_in_ref, s_out_ref)):
        high = ref[...].astype(BF16).astype(F32)
        state[4 * k : 4 * k + 2] = high
        state[4 * k + 2 : 4 * k + 4] = ref[...] - high
    rows_ref[:, 6 * R :] = state[...].astype(BF16)


def terms_kernel(coded_ref, logit_ref, cot_ref, rec_ref, bound_ref, term_ref):
    sig = jax.nn.sigmoid(logit_ref[...].astype(F32))
    gate_cot = (
        cot_ref[...].astype(F32) * (1.0 - bound_ref[...][None, :]) * sig * (1.0 - sig)
    ).astype(BF16)
    n_x, wide, tokens = coded_ref.shape
    units, width = rec_ref.shape[1], wide // 2
    rows = term_ref.shape[1]
    for at, part in ((0, gate_cot), (1, rec_ref[...])):
        coded = coded_ref[:, at * width : (at + 1) * width].reshape(n_x * width, tokens)
        term = dot(coded, part, NN)
        for k in range(term_ref.shape[0]):
            term_ref[k, :, at * units : (at + 1) * units] = term[k * rows : (k + 1) * rows]


def totals_kernel(terms_ref, total_ref, rounded_ref, squares_ref):
    total = terms_ref[0].astype(F32)
    for k in range(1, terms_ref.shape[0]):
        total = total + terms_ref[k].astype(F32)
    total_ref[...] = total
    rounded_ref[...] = total.astype(BF16)
    squares_ref[...] = jnp.full(squares_ref.shape, jnp.sum(total * total), F32)


def update_kernel(
    squares_ref,
    low_ref,
    term_ref,
    state_ref,
    rows_ref,
    sorted_ref,
    w_in_ref,
    w_out_ref,
    m_in_ref,
    m_out_ref,
    s_in_ref,
    s_out_ref,
    copy_in_ref,
    copy_out_ref,
    w_in_new_ref,
    w_out_new_ref,
    m_in_new_ref,
    m_out_new_ref,
    s_in_new_ref,
    s_out_new_ref,
    state,
    low,
    step,
    step_in,
    step_out,
):
    units = w_in_ref.shape[1]

    @pl.when(pl.program_id(0) == 0)
    def _():
        count, half = state.shape[1] // 16, R // 2
        total = jnp.sum(squares_ref[...], axis=0)
        clip = jnp.minimum(1.0, jnp.sqrt(jnp.float32(2 * R * HW)) * lax.rsqrt(total + 1e-06))
        for lane in range(0, units, 128):
            state[lane // 128] = state_ref[:, lane : lane + 128].astype(F32)
        n_z, blocks = count // 16, 16
        for lane in range(0, 2 * units, 128):
            low[0, lane // 128] = low_ref[:, lane : lane + 128].astype(F32)
            for p in range(2):
                for z in range(n_z):
                    low[1, lane // 128, pl.ds(p * half + z * blocks, blocks), :] = low[
                        0, lane // 128, pl.ds(p * n_z + z, blocks, stride=2 * n_z), :
                    ]
        for side in range(2):
            for lane in range(0, units, 128):
                for p in range(2):
                    row = lambda k: state[lane // 128, pl.ds(4 * side + p + k, count, stride=16), :]
                    at, to = pl.ds(p * half, half), pl.ds(lane, 128)
                    grad = clip * low[1, (side * units + lane) // 128, at, :]
                    moment = 0.8 * (row(0) + row(2)) + 0.2 * grad
                    second = 0.9 * (row(8) + row(10)) + 0.1 * grad * grad
                    moved = 0.01 * (moment / (jnp.sqrt(second) + 1e-08))
                    step[side, at, to] = moved
        step_in[:R], step_in[R:] = halves(step[0])
        step_out[:, :R], step_out[:, R:] = halves(step[1].T)
        own = w_in_ref.shape[0]
        w_in_new_ref[...] = w_in_ref[...] - dot(twice(sorted_ref[:own]), step_in[...], NN)
        high, rest = halves(step[1])
        mine = sorted_ref[own:]
        w_out_new_ref[...] = w_out_ref[...] - (dot(mine, high, NN) + dot(mine, rest, NN))
        for p in range(2):
            grad = term_ref[pl.ds(p * n_z + lax.axis_index(Z), 1), :]
            grad = grad * jnp.concatenate([clip] * (2 * units // 128), axis=1)
            for g, m, s, m_new, s_new in (
                (grad[:, :units], m_in_ref, s_in_ref, m_in_new_ref, s_in_new_ref),
                (grad[:, units:], m_out_ref, s_out_ref, m_out_new_ref, s_out_new_ref),
            ):
                m_new[p : p + 1] = 0.8 * m[p : p + 1] + 0.2 * g
                s_new[p : p + 1] = 0.9 * s[p : p + 1] + 0.1 * g * g

    w = lambda k: rows_ref[:, k * R : (k + 1) * R]
    moved = dot(twice(w(0)), step_in[...], NN)
    copy_in_ref[...] = (w(2).astype(F32) + w(3).astype(F32) - moved).astype(BF16)
    moved = dot(step_out[...], twice(w(1)), NT)
    copy_out_ref[...] = ((w(4).astype(F32) + w(5).astype(F32)).T - moved).astype(BF16)


def update(squares, low, term, rows, sorted_both, weight_in, weight_out, moments):
    d, units, tile = rows.shape[0], weight_in.shape[1], 512
    whole = lambda a: pl.BlockSpec(a.shape, lambda i: (0,) * a.ndim)
    small = (weight_in, weight_out, *moments)
    return call(
        update_kernel,
        (squares, low, term, rows, rows, sorted_both, *small),
        [
            jax.ShapeDtypeStruct((d, units), BF16),
            jax.ShapeDtypeStruct((units, d), BF16),
            *[jax.ShapeDtypeStruct(a.shape, F32) for a in small],
        ],
        scratch=[
            pltpu.VMEM((units // 128, d, 128), F32),
            pltpu.VMEM((2, 2 * units // 128, R, 128), F32),
            pltpu.VMEM((2, R, units), F32),
            pltpu.VMEM((2 * R, units), BF16),
            pltpu.VMEM((units, 2 * R), BF16),
        ],
        flops=14 * d * R * units,
        grid=(d // tile,),
        in_specs=[
            whole(squares),
            whole(low),
            whole(term),
            pl.BlockSpec((d, R), lambda i: (0, 6)),
            pl.BlockSpec((tile, 6 * R), lambda i: (i, 0)),
            whole(sorted_both),
            *[whole(a) for a in small],
        ],
        out_specs=[
            pl.BlockSpec((tile, units), lambda i: (i, 0)),
            pl.BlockSpec((units, tile), lambda i: (0, i)),
            *[whole(a) for a in small],
        ],
        compiler_params=pltpu.CompilerParams(vmem_limit_bytes=60 * 2**20),
    )


def body(
    saved_input,
    output_cotangent,
    recurrent_output,
    forget_logit,
    forget_cotangent,
    lower_bound,
    basis_in,
    basis_out,
    moment_in,
    second_in,
    moment_out,
    second_out,
    weight_in,
    weight_out,
):
    n_z, n_y, n_c, n_x = (lax.axis_size(a) for a in (Z, Y, C, X))
    n_fs = n_z * n_y * n_c
    units, own = recurrent_output.shape[1], basis_in.shape[0]
    width = R // n_x
    after, before = rank_orders(n_z, n_y, n_c)
    quarters = np.concatenate([before.reshape(n_x, width)] * 2, axis=1).astype(np.float32)
    after = after.astype(np.float32)[None, :]

    block, sorted_both, payload = call(
        pack_kernel,
        (
            jnp.asarray(quarters),
            jnp.asarray(after),
            basis_in,
            basis_out,
            moment_in,
            moment_out,
            second_in,
            second_out,
            weight_in,
            weight_out.T,
        ),
        [
            jax.ShapeDtypeStruct((n_z, own, 2 * width), BF16),
            jax.ShapeDtypeStruct((2 * own, R), BF16),
            jax.ShapeDtypeStruct((own, 7 * R), BF16),
        ],
        scratch=[pltpu.VMEM((16, units), F32)],
    )

    rows = lax.all_gather(payload, FS, axis=0, tiled=True)

    full = lax.all_to_all(block, Z, 0, 0)
    full = (full.astype(F32) * 1024.0).astype(jnp.float16)
    full = lax.all_gather(full, (Y, C), axis=0, tiled=False)
    full = jnp.moveaxis(full, 0, 1).astype(F32) * (1.0 / 1024.0)
    full = full.astype(BF16).reshape(-1, 2 * width)

    first = lax.broadcasted_iota(jnp.int32, (2 * width, 1), 0) < width
    part = jnp.where(
        first,
        dot(full, saved_input, ((0,), (1,))),
        dot(full, output_cotangent, ((0,), (1,))),
    ).astype(BF16)
    coded = lax.all_gather(part, X, axis=0, tiled=False)

    term = call(
        terms_kernel,
        (coded, forget_logit, forget_cotangent, recurrent_output, lower_bound),
        jax.ShapeDtypeStruct((n_c, R // n_c, 2 * units), F32),
        flops=4 * R * units * recurrent_output.shape[0],
    )

    term = lax.all_to_all(term, C, 0, 0)
    term = (term[0] + term[1]).astype(BF16).reshape(n_y, R // n_c // n_y, -1)
    term = jnp.sum(lax.all_to_all(term, Y, 0, 0).astype(F32), axis=0).astype(BF16)
    term, rounded, squares = call(
        totals_kernel,
        (lax.all_gather(term, Z, axis=0, tiled=False),),
        [
            jax.ShapeDtypeStruct(term.shape, F32),
            jax.ShapeDtypeStruct(term.shape, BF16),
            jax.ShapeDtypeStruct((n_y * n_c * n_x, 1, 128), F32),
        ],
    )
    squares = lax.all_to_all(squares, (Y, C, X), 0, 0, tiled=True)
    low = lax.all_gather(rounded, (Y, C), axis=0, tiled=True)
    moments = (moment_in, moment_out, second_in, second_out)
    new = update(squares, low, term, rows, sorted_both, weight_in, weight_out.T, moments)
    copy_in, copy_out, weight_in, weight_out, moment_in, moment_out, second_in, second_out = new
    return (
        moment_in,
        second_in,
        moment_out,
        second_out,
        weight_in,
        weight_out.T,
        copy_in,
        copy_out,
    )


def solution(mesh):
    finer = Mesh(mesh.devices.reshape(12, 8, 2, mesh.shape["tp"]), (Z, Y, C, X))
    return jax.shard_map(
        body,
        mesh=finer,
        in_specs=(
            P(FS, None),
            P(FS, None),
            P(FS, X),
            P(FS, X),
            P(FS, X),
            P(X),
            P(FS, None),
            P(FS, None),
            P(FS, X),
            P(FS, X),
            P(FS, X),
            P(FS, X),
            P(FS, X),
            P(X, FS),
        ),
        out_specs=(
            P(FS, X),
            P(FS, X),
            P(FS, X),
            P(FS, X),
            P(FS, X),
            P(X, FS),
            P(None, X),
            P(X, None),
        ),
        check_vma=False,
    )
```

```python
import functools

import jax
import jax.numpy as jnp
import numpy as np
from jax import lax
from jax.experimental import pallas as pl
from jax.experimental.pallas import tpu as pltpu
from jax.sharding import Mesh
from jax.sharding import PartitionSpec as P

HW = 1536
R = 384
Z, Y, C, X = "fs_0", "fs_1", "fs_2", "tp"
FS = (Z, Y, C)
F32, BF16 = jnp.float32, jnp.bfloat16


def rank_orders(n_z, n_y, n_c):
    n_fs = n_z * n_y * n_c
    at = np.arange(R)
    steps = 2 * (at % n_fs) + at // n_fs
    c, y, p, z = np.unravel_index(at, (n_c, n_y, 2, n_z))
    return steps, 2 * ((z * n_y + y) * n_c + c) + p


def dot(a, b, dims):
    return lax.dot_general(a, b, (dims, ((), ())), preferred_element_type=F32)


NN, NT = ((1,), (0,)), ((1,), (1,))


def halves(a):
    high = a.astype(BF16)
    return high, (a - high.astype(F32)).astype(BF16)


def twice(a):
    return jnp.concatenate([a, a], axis=1)


def call(kernel, args, out_shape, scratch=(), flops=10**6, limit=12 * 2**20, **more):
    return pl.pallas_call(
        kernel,
        out_shape=out_shape,
        scratch_shapes=scratch,
        cost_estimate=pl.CostEstimate(flops=flops, bytes_accessed=10**5, transcendentals=0),
        compiler_params=pltpu.CompilerParams(vmem_limit_bytes=limit),
        **more,
    )(*args)


def pack_kernel(
    quarters_ref,
    after_ref,
    in_ref,
    out_ref,
    m_in_ref,
    m_out_ref,
    s_in_ref,
    s_out_ref,
    w_in_ref,
    w_out_ref,
    block_ref,
    sorted_ref,
    rows_ref,
    state,
):
    n_x, wide = quarters_ref.shape
    mine = lax.broadcasted_iota(jnp.int32, (n_x, wide), 0) == lax.axis_index(X)
    ranks = jnp.sum(jnp.where(mine, quarters_ref[...], 0.0), axis=0, keepdims=True)
    rank = lax.broadcasted_iota(jnp.int32, (R, wide), 0).astype(F32)
    lane = lax.broadcasted_iota(jnp.int32, (R, wide), 1)
    hot = jnp.where(rank == ranks, 1.0, 0.0)
    hot_in = jnp.where(lane < wide // 2, hot, 0.0).astype(BF16)
    hot_out = jnp.where(lane < wide // 2, 0.0, hot).astype(BF16)
    block = (dot(in_ref[...], hot_in, NN) + dot(out_ref[...], hot_out, NN)).astype(BF16)
    for k in range(block_ref.shape[0]):
        block_ref[k] = block
    rank = lax.broadcasted_iota(jnp.int32, (R, R), 0).astype(F32)
    hot = jnp.where(rank == after_ref[...], 1.0, 0.0).astype(BF16)
    own = in_ref.shape[0]
    for k, ref in enumerate((in_ref, out_ref)):
        piece = dot(ref[...], hot, NN).astype(BF16)
        sorted_ref[k * own : (k + 1) * own] = piece
        rows_ref[:, k * R : (k + 1) * R] = piece
    for k, piece in enumerate(halves(w_in_ref[...])):
        rows_ref[:, (2 + k) * R : (3 + k) * R] = piece
    for k, piece in enumerate(halves(w_out_ref[...])):
        rows_ref[:, (4 + k) * R : (5 + k) * R] = piece
    for k, ref in enumerate((m_in_ref, m_out_ref, s_in_ref, s_out_ref)):
        high = ref[...].astype(BF16).astype(F32)
        state[4 * k : 4 * k + 2] = high
        state[4 * k + 2 : 4 * k + 4] = ref[...] - high
    rows_ref[:, 6 * R :] = state[...].astype(BF16)


def terms_kernel(coded_ref, logit_ref, cot_ref, rec_ref, bound_ref, term_ref):
    sig = jax.nn.sigmoid(logit_ref[...].astype(F32))
    gate_cot = (
        cot_ref[...].astype(F32) * (1.0 - bound_ref[...][None, :]) * sig * (1.0 - sig)
    ).astype(BF16)
    n_x, wide, tokens = coded_ref.shape
    units, width = rec_ref.shape[1], wide // 2
    rows = term_ref.shape[1]
    for at, part in ((0, gate_cot), (1, rec_ref[...])):
        coded = coded_ref[:, at * width : (at + 1) * width].reshape(n_x * width, tokens)
        term = dot(coded, part, NN)
        for k in range(term_ref.shape[0]):
            term_ref[k, :, at * units : (at + 1) * units] = term[k * rows : (k + 1) * rows]


def totals_kernel(terms_ref, total_ref, rounded_ref, squares_ref):
    total = terms_ref[0].astype(F32)
    for k in range(1, terms_ref.shape[0]):
        total = total + terms_ref[k].astype(F32)
    total_ref[...] = total
    rounded_ref[...] = total.astype(BF16)
    squares_ref[...] = jnp.full(squares_ref.shape, jnp.sum(total * total), F32)


def update_kernel(
    squares_ref,
    low_ref,
    term_ref,
    state_ref,
    rows_ref,
    sorted_ref,
    w_in_ref,
    w_out_ref,
    m_in_ref,
    m_out_ref,
    s_in_ref,
    s_out_ref,
    copy_in_ref,
    copy_out_ref,
    w_in_new_ref,
    w_out_new_ref,
    m_in_new_ref,
    m_out_new_ref,
    s_in_new_ref,
    s_out_new_ref,
    state,
    low,
    step,
    step_in,
    step_out,
):
    units = w_in_ref.shape[1]

    @pl.when(pl.program_id(0) == 0)
    def _():
        count, half = state.shape[1] // 16, R // 2
        total = jnp.sum(squares_ref[...], axis=0)
        clip = jnp.minimum(1.0, jnp.sqrt(jnp.float32(2 * R * HW)) * lax.rsqrt(total + 1e-06))
        for lane in range(0, units, 128):
            state[lane // 128] = state_ref[:, lane : lane + 128].astype(F32)
        n_z, blocks = count // 16, 16
        for lane in range(0, 2 * units, 128):
            low[0, lane // 128] = low_ref[:, lane : lane + 128].astype(F32)
            for p in range(2):
                for z in range(n_z):
                    low[1, lane // 128, pl.ds(p * half + z * blocks, blocks), :] = low[
                        0, lane // 128, pl.ds(p * n_z + z, blocks, stride=2 * n_z), :
                    ]
        for side in range(2):
            for lane in range(0, units, 128):
                for p in range(2):
                    row = lambda k: state[lane // 128, pl.ds(4 * side + p + k, count, stride=16), :]
                    at, to = pl.ds(p * half, half), pl.ds(lane, 128)
                    grad = clip * low[1, (side * units + lane) // 128, at, :]
                    moment = 0.8 * (row(0) + row(2)) + 0.2 * grad
                    second = 0.9 * (row(8) + row(10)) + 0.1 * grad * grad
                    moved = 0.01 * (moment / (jnp.sqrt(second) + 1e-08))
                    step[side, at, to] = moved
        step_in[:R], step_in[R:] = halves(step[0])
        step_out[:, :R], step_out[:, R:] = halves(step[1].T)
        own = w_in_ref.shape[0]
        w_in_new_ref[...] = w_in_ref[...] - dot(twice(sorted_ref[:own]), step_in[...], NN)
        high, rest = halves(step[1])
        mine = sorted_ref[own:]
        w_out_new_ref[...] = w_out_ref[...] - (dot(mine, high, NN) + dot(mine, rest, NN))
        for p in range(2):
            grad = term_ref[pl.ds(p * n_z + lax.axis_index(Z), 1), :]
            grad = grad * jnp.concatenate([clip] * (2 * units // 128), axis=1)
            for g, m, s, m_new, s_new in (
                (grad[:, :units], m_in_ref, s_in_ref, m_in_new_ref, s_in_new_ref),
                (grad[:, units:], m_out_ref, s_out_ref, m_out_new_ref, s_out_new_ref),
            ):
                m_new[p : p + 1] = 0.8 * m[p : p + 1] + 0.2 * g
                s_new[p : p + 1] = 0.9 * s[p : p + 1] + 0.1 * g * g

    w = lambda k: rows_ref[:, k * R : (k + 1) * R]
    moved = dot(twice(w(0)), step_in[...], NN)
    copy_in_ref[...] = (w(2).astype(F32) + w(3).astype(F32) - moved).astype(BF16)
    moved = dot(step_out[...], twice(w(1)), NT)
    copy_out_ref[...] = ((w(4).astype(F32) + w(5).astype(F32)).T - moved).astype(BF16)


def update(squares, low, term, rows, sorted_both, weight_in, weight_out, moments):
    d, units, tile = rows.shape[0], weight_in.shape[1], 512
    whole = lambda a: pl.BlockSpec(a.shape, lambda i: (0,) * a.ndim)
    small = (weight_in, weight_out, *moments)
    return call(
        update_kernel,
        (squares, low, term, rows, rows, sorted_both, *small),
        [
            jax.ShapeDtypeStruct((d, units), BF16),
            jax.ShapeDtypeStruct((units, d), BF16),
            *[jax.ShapeDtypeStruct(a.shape, F32) for a in small],
        ],
        scratch=[
            pltpu.VMEM((units // 128, d, 128), F32),
            pltpu.VMEM((2, 2 * units // 128, R, 128), F32),
            pltpu.VMEM((2, R, units), F32),
            pltpu.VMEM((2 * R, units), BF16),
            pltpu.VMEM((units, 2 * R), BF16),
        ],
        flops=14 * d * R * units,
        grid=(d // tile,),
        in_specs=[
            whole(squares),
            whole(low),
            whole(term),
            pl.BlockSpec((d, R), lambda i: (0, 6)),
            pl.BlockSpec((tile, 6 * R), lambda i: (i, 0)),
            whole(sorted_both),
            *[whole(a) for a in small],
        ],
        out_specs=[
            pl.BlockSpec((tile, units), lambda i: (i, 0)),
            pl.BlockSpec((units, tile), lambda i: (0, i)),
            *[whole(a) for a in small],
        ],
        limit=60 * 2**20,
    )


def body(
    saved_input,
    output_cotangent,
    recurrent_output,
    forget_logit,
    forget_cotangent,
    lower_bound,
    basis_in,
    basis_out,
    moment_in,
    second_in,
    moment_out,
    second_out,
    weight_in,
    weight_out,
):
    n_z, n_y, n_c, n_x = (lax.axis_size(a) for a in (Z, Y, C, X))
    n_fs = n_z * n_y * n_c
    units, own = recurrent_output.shape[1], basis_in.shape[0]
    width = R // n_x
    after, before = rank_orders(n_z, n_y, n_c)
    quarters = np.concatenate([before.reshape(n_x, width)] * 2, axis=1).astype(np.float32)
    after = after.astype(np.float32)[None, :]

    block, sorted_both, payload = call(
        pack_kernel,
        (
            jnp.asarray(quarters),
            jnp.asarray(after),
            basis_in,
            basis_out,
            moment_in,
            moment_out,
            second_in,
            second_out,
            weight_in,
            weight_out.T,
        ),
        [
            jax.ShapeDtypeStruct((n_z, own, 2 * width), BF16),
            jax.ShapeDtypeStruct((2 * own, R), BF16),
            jax.ShapeDtypeStruct((own, 7 * R), BF16),
        ],
        scratch=[pltpu.VMEM((16, units), F32)],
        limit=60 * 2**20,
    )

    rows = lax.all_gather(payload, FS, axis=0, tiled=True)

    full = lax.all_to_all(block, Z, 0, 0)
    full = (full.astype(F32) * 1024.0).astype(jnp.float16)
    full = lax.all_gather(full, (Y, C), axis=0, tiled=False)
    full = jnp.moveaxis(full, 0, 1).astype(F32) * (1.0 / 1024.0)
    full = full.astype(BF16).reshape(-1, 2 * width)

    first = lax.broadcasted_iota(jnp.int32, (2 * width, 1), 0) < width
    part = jnp.where(
        first,
        dot(full, saved_input, ((0,), (1,))),
        dot(full, output_cotangent, ((0,), (1,))),
    ).astype(BF16)
    coded = lax.all_gather(part, X, axis=0, tiled=False)

    term = call(
        terms_kernel,
        (coded, forget_logit, forget_cotangent, recurrent_output, lower_bound),
        jax.ShapeDtypeStruct((n_c, R // n_c, 2 * units), F32),
        flops=4 * R * units * recurrent_output.shape[0],
    )

    term = lax.all_to_all(term, C, 0, 0)
    term = (term[0] + term[1]).astype(BF16).reshape(n_y, R // n_c // n_y, -1)
    term = jnp.sum(lax.all_to_all(term, Y, 0, 0).astype(F32), axis=0).astype(BF16)
    term, rounded, squares = call(
        totals_kernel,
        (lax.all_gather(term, Z, axis=0, tiled=False),),
        [
            jax.ShapeDtypeStruct(term.shape, F32),
            jax.ShapeDtypeStruct(term.shape, BF16),
            jax.ShapeDtypeStruct((n_y * n_c * n_x, 1, 128), F32),
        ],
    )
    squares = lax.all_to_all(squares, (Y, C, X), 0, 0, tiled=True)
    low = lax.all_gather(rounded, (Y, C), axis=0, tiled=True)
    moments = (moment_in, moment_out, second_in, second_out)
    new = update(squares, low, term, rows, sorted_both, weight_in, weight_out.T, moments)
    copy_in, copy_out, weight_in, weight_out, moment_in, moment_out, second_in, second_out = new
    return (
        moment_in,
        second_in,
        moment_out,
        second_out,
        weight_in,
        weight_out.T,
        copy_in,
        copy_out,
    )


def solution(mesh):
    finer = Mesh(mesh.devices.reshape(12, 8, 2, mesh.shape["tp"]), (Z, Y, C, X))
    return jax.shard_map(
        body,
        mesh=finer,
        in_specs=(
            P(FS, None),
            P(FS, None),
            P(FS, X),
            P(FS, X),
            P(FS, X),
            P(X),
            P(FS, None),
            P(FS, None),
            P(FS, X),
            P(FS, X),
            P(FS, X),
            P(FS, X),
            P(FS, X),
            P(X, FS),
        ),
        out_specs=(
            P(FS, X),
            P(FS, X),
            P(FS, X),
            P(FS, X),
            P(FS, X),
            P(X, FS),
            P(None, X),
            P(X, None),
        ),
        check_vma=False,
    )
```
